1024 devices in a mesh: gr: 4 (over z_hi), sp: 32 (over z_lo, y), tp: 8 (over x, core).
Axes of the slice: x: 4, y: 4, z: 32 (z_hi: 4, z_lo: 8; z = z_hi * 8 + z_lo), core: 2. Of those that a mesh axis runs over, the one named last changes fastest.
Arguments:
- prompt: bfloat16 [16, 4096, 4096], P('gr', 'sp'), may hold values from -16 to 16
- forget_weight: bfloat16 [4096, 2048], P(None, 'tp'), may hold values from -0.09375 to 0.09375
- value_weight: bfloat16 [4096, 2048], P(None, 'tp'), may hold values from -0.09375 to 0.09375
- leak: float32 [2048], P('tp'), may hold values from 0 to 1, as said below
- query: bfloat16 [16, 2048], P('gr', 'tp'), may hold values from -6 to 6
- next_input: bfloat16 [16, 4096], P('gr'), may hold values from -6 to 6
- read_gain: float32 [2048], P('tp'), may hold values from 0.1 to 1.9
Outputs:
- state_cache: bfloat16 [16, 16, 128, 128], P('gr', 'tp', 'sp')
- read_out: bfloat16 [16, 2048], P('gr', 'tp')
The draws below stay inside these ranges and needn't reach their ends.
Inputs may be any that keep to these rules, and one draw needn't show every extreme that they name: `leak`: positive, at most one half.
All inputs are finite; a program needn't handle non-finite values.
Results may differ from the reference program's by a relative error of at most 0.0062.
Values sent between devices are 32-bit elements; how exact they have to be, the bound alone decides.
A program may use at most 64 MiB of HBM per device.

```python
import jax
import jax.numpy as jnp
from jax import lax

D = 4096
HEADS = 16
DK = 128
DV = 128
POS_DEV = 128
SEQS = 16
LEN = 4096
N_SP = 32


def draw_prompt(key, part):
    key_scale = jax.random.fold_in(key, 11)
    key_main = jax.random.fold_in(key, 12)
    blocks = LEN // 8
    log_scale = jax.random.uniform(key_scale, (SEQS, blocks, 1), jnp.float32, jnp.log(0.4), jnp.log(2.5))
    scale = jnp.repeat(jnp.exp(log_scale), 8, axis=1)
    values = jax.random.normal(key_main, (SEQS, LEN, D), jnp.float32) * scale
    return jnp.clip(values, -16.0, 16.0).astype(jnp.bfloat16)


def draw_leak(key, part):
    key_main = jax.random.fold_in(key, 21)
    length = float(LEN)
    low = 0.4 / length
    high = min(120.0 / length, 0.5)
    spread = jax.random.uniform(key_main, (HEADS * DK,), jnp.float32)
    return jnp.exp(jnp.log(low) + spread * (jnp.log(high) - jnp.log(low))).astype(jnp.float32)


def steps_of(rng, extent, pieces, smallest, largest):
    def one(axis_at, parts):
        steps = jax.random.uniform(jax.random.fold_in(jax.random.fold_in(rng, 6), axis_at), (parts,), jnp.float32, smallest / len(pieces), largest / len(pieces))
        return jnp.repeat(jnp.exp(steps), extent[axis_at] // parts).reshape((-1,) + (1,) * (len(extent) - axis_at - 1))

    level = one(*pieces[0])
    for cut in pieces[1:]:
        level = level * one(*cut)
    return level


def normal_values(key, shape, width, most, split=(), dtype=jnp.bfloat16):
    drawn = width * jax.random.normal(key, shape, jnp.float32)
    if split:
        drawn = drawn * steps_of(key, shape, split, -0.22, 0.18)
    return jnp.clip(drawn, -most, most).astype(dtype)


def setup_inputs(seed: int = 0) -> dict:
    arg_keys = jax.random.split(jax.random.key(seed), 8)
    return {
        "prompt": draw_prompt(jax.random.fold_in(arg_keys[7], 71), 0),
        "forget_weight": normal_values(arg_keys[1], (D, HEADS * DK), D ** -0.5, 0.09375, ((1, 8),)),
        "value_weight": normal_values(arg_keys[2], (D, HEADS * DV), D ** -0.5, 0.09375, ((1, 8),)),
        "leak": draw_leak(jax.random.fold_in(arg_keys[7], 71), 0),
        "query": normal_values(arg_keys[4], (SEQS, HEADS * DK), 1.0, 6.0, ((0, 4), (1, 8))),
        "next_input": normal_values(arg_keys[5], (SEQS, D), 1.0, 6.0, ((0, 4),)),
        "read_gain": jnp.clip(1.0 + 0.18 * jax.random.normal(arg_keys[6], (HEADS * DV,), jnp.float32), 0.1, 1.9),
    }


def sequence_state(seq_rows, forget_weight, value_weight, leak):
    gate_pre = jnp.dot(seq_rows, forget_weight, preferred_element_type=jnp.float32)
    values = jnp.dot(seq_rows, value_weight, preferred_element_type=jnp.float32).astype(jnp.bfloat16)
    inflow = leak * jax.nn.sigmoid(-gate_pre)
    decay_log = jnp.log1p(-inflow)
    inflow = inflow.reshape(N_SP, POS_DEV, HEADS, DK)
    decay_log = decay_log.reshape(N_SP, POS_DEV, HEADS, DK)
    values = values.reshape(N_SP, POS_DEV, HEADS, DV)
    seg_cum = jnp.cumsum(decay_log, axis=1)
    seg_total = seg_cum[:, -1]
    weighted = (inflow * jnp.exp(seg_total[:, None] - seg_cum)).astype(jnp.bfloat16)
    seg_state = jnp.einsum('nphk,nphv->nhkv', weighted.astype(jnp.float32), values.astype(jnp.float32))
    later = jnp.cumsum(seg_total[::-1], axis=0)[::-1] - seg_total
    return lax.optimization_barrier(jnp.sum(jnp.exp(later)[..., None] * seg_state, axis=0))

def reference(prompt, forget_weight, value_weight, leak, query, next_input, read_gain):
    states = lax.map(lambda rows: sequence_state(rows, forget_weight, value_weight, leak), prompt)
    next_pre = jnp.dot(next_input, forget_weight, preferred_element_type=jnp.float32).reshape(SEQS, HEADS, DK)
    next_values = jnp.dot(next_input, value_weight, preferred_element_type=jnp.float32).astype(jnp.bfloat16)
    next_values = next_values.astype(jnp.float32).reshape(SEQS, HEADS, DV)
    next_inflow = leak.reshape(HEADS, DK) * jax.nn.sigmoid(-next_pre)
    next_forget = 1.0 - next_inflow
    read_state = next_forget[..., None] * states + next_inflow[..., None] * next_values[:, :, None, :]
    queries = query.astype(jnp.float32).reshape(SEQS, HEADS, DK)
    raw_read = lax.optimization_barrier(jnp.sum(queries[..., None] * read_state, axis=2))
    scaled = raw_read * lax.rsqrt(lax.optimization_barrier(jnp.mean(raw_read * raw_read, axis=-1, keepdims=True)) + 1e-06)
    read_out = (scaled * read_gain.reshape(HEADS, DV)).astype(jnp.bfloat16).reshape(SEQS, HEADS * DV)
    return (states.astype(jnp.bfloat16), read_out)
```

```python
import functools

import jax
import jax.numpy as jnp
from jax import lax
from jax.experimental import pallas as pl
from jax.experimental.pallas import tpu as pltpu
from jax.sharding import PartitionSpec as P

MESH = pl.DeviceIdType.MESH
F32 = jnp.float32
BF16 = jnp.bfloat16
DK = 128
DV = 128
NY = 4
CHUNKS = 4
EPS = 1e-6


def dot(a, b, contract=((1,), (0,))):
    return lax.dot_general(a, b, (contract, ((), ())), preferred_element_type=F32)


def halves(x):
    high = x.astype(BF16)
    return high, (x - high.astype(F32)).astype(BF16)


def kernel(
    nz, prompt, fw, vw, leak_in, query_in, next_in, gain_in, cache_out, read_out,
    x, wf, wv, leak, query, nexts, gain, acc, inflow, decays, vals, packed,
    ys, split, r1, q2, r2, zs, zr, yt, zt, yr, rz, cols, cols_src,
    x_sem, wf_sem, wv_sem, small_sem,
    yt_send, yt_recv, zt_send, zt_recv, r1_send, r1_recv, r2_send, r2_recv,
    zr_send, zr_recv, yr_send, yr_recv, rz_send, rz_recv,
):
    seqs = query.shape[0]
    span = x.shape[0] // seqs
    heads = query.shape[1] // DK
    depth = x.shape[1]
    step = depth // CHUNKS
    me = lax.axis_index("sp")
    z = lax.div(me, NY)
    y = lax.rem(me, NY)

    def at(zz, yy):
        return {"sp": zz * NY + yy}

    y_peers = [lax.rem(y + d, NY) for d in range(1, NY)]
    z_peers = [lax.rem(z + d, nz) for d in range(1, nz)]

    barrier = pltpu.get_barrier_semaphore()
    for p in y_peers:
        pl.semaphore_signal(barrier, inc=1, device_id=at(z, p), device_id_type=MESH)
    for p in z_peers:
        pl.semaphore_signal(barrier, inc=1, device_id=at(p, y), device_id_type=MESH)

    def cut(c):
        return pl.ds(c * step, step)

    x_copies = [pltpu.make_async_copy(prompt.at[:, cut(c)], x.at[:, cut(c)], x_sem.at[c]) for c in range(CHUNKS)]
    f_copies = [pltpu.make_async_copy(fw.at[cut(c)], wf.at[cut(c)], wf_sem.at[c]) for c in range(CHUNKS)]
    v_copies = [pltpu.make_async_copy(vw.at[cut(c)], wv.at[cut(c)], wv_sem.at[c]) for c in range(CHUNKS)]
    small = [
        pltpu.make_async_copy(src, dst, small_sem.at[i])
        for i, (src, dst) in enumerate(((leak_in, leak), (query_in, query), (next_in, nexts), (gain_in, gain)))
    ]
    for c in range(CHUNKS):
        f_copies[c].start()
        x_copies[c].start()
    for copy in small:
        copy.start()

    def remote(src, dst, send, recv, to):
        return pltpu.make_async_remote_copy(
            src_ref=src, dst_ref=dst, send_sem=send, recv_sem=recv, device_id=to, device_id_type=MESH
        )

    for c in range(CHUNKS):
        f_copies[c].wait()
        x_copies[c].wait()
        part = dot(x[:, cut(c)], wf[cut(c), :])
        if c == 0:
            acc[...] = part
            for copy in v_copies:
                copy.start()
        else:
            acc[...] += part
    for copy in small:
        copy.wait()

    leak_row = leak[...]
    totals = []
    for s in range(seqs):
        rows = pl.ds(s * span, span)
        flow = leak_row * jax.nn.sigmoid(-acc[rows, :])
        inflow[rows, :] = flow
        log = jnp.log(1.0 - flow)
        high, low = halves(log)
        decays[s, 0:span, :] = high
        decays[s, span:2 * span, :] = low
        totals.append(jnp.sum(log, axis=0, keepdims=True))

    def by_head(rows):
        return jnp.concatenate([rows[:, h * DK:(h + 1) * DK] for h in range(heads)], axis=0)

    yt[y] = by_head(jnp.concatenate(totals, axis=0))
    pl.semaphore_wait(barrier, NY - 1 + nz - 1)
    yt_copies = [
        remote(yt.at[y], yt.at[y], yt_send.at[i], yt_recv.at[y], at(z, p)) for i, p in enumerate(y_peers)
    ]
    for copy in yt_copies:
        copy.start()

    for c in range(CHUNKS):
        v_copies[c].wait()
        part = dot(x[:, cut(c)], wv[cut(c), :])
        if c == 0:
            acc[...] = part
        elif c < CHUNKS - 1:
            acc[...] += part
        else:
            vals[...] = (acc[...] + part).astype(BF16)

    for p in y_peers:
        remote(yt.at[p], yt.at[p], yt_send.at[0], yt_recv.at[p], at(z, p)).wait_recv()
    all_y = [yt[j] for j in range(NY)]
    later_y = sum(jnp.where(y < j, all_y[j], 0.0) for j in range(1, NY))
    zt[z] = sum(all_y[1:], all_y[0])
    zt_copies = [
        remote(zt.at[z], zt.at[z], zt_send.at[i], zt_recv.at[z], at(p, y)) for i, p in enumerate(z_peers)
    ]
    for copy in zt_copies:
        copy.start()

    rows_at = lax.broadcasted_iota(jnp.int32, (span, 2 * span), 0)
    cols_at = lax.rem(lax.broadcasted_iota(jnp.int32, (span, 2 * span), 1), span)
    upper = jnp.where(cols_at > rows_at, 1.0, 0.0).astype(BF16)

    first, second = [], []
    for s in range(seqs):
        pair = y + 1 - 2 * lax.rem(y, 2)
        across = NY - 1 - y
        first.append(pair if s % 2 == 0 else across)
        second.append(across if s % 2 == 0 else pair)

    r1_copies = []
    for s in range(seqs):
        rows = pl.ds(s * span, span)
        later_row = jnp.concatenate([later_y[h * seqs + s:h * seqs + s + 1, :] for h in range(heads)], axis=1)
        left = dot(upper, decays[s]) + later_row
        weighted = (inflow[rows, :] * jnp.exp(left)).astype(BF16)
        for h in range(heads):
            lanes = slice(h * DK, (h + 1) * DK)
            state = dot(weighted[:, lanes], vals[rows, lanes], ((0,), (0,)))
            high, low = halves(state)
            split[s, 0:DK, lanes] = high
            split[s, DK:2 * DK, lanes] = low
            own = DK // (NY * nz)
            for zz in range(nz):
                for yy in range(NY):
                    k = (zz * NY + yy) * own
                    ys[yy, s, zz, h * own:(h + 1) * own, :] = state[k:k + own, :]
        p = first[s]
        beyond = NY - 1 - p if s % 2 == 0 else p + 1 - 2 * lax.rem(p, 2)
        for i, target in enumerate((beyond, p)):
            copy = remote(ys.at[target, s], r1.at[s, 1 - i], r1_send.at[s, i], r1_recv.at[s, 1 - i], at(z, p))
            copy.start()
            r1_copies.append(copy)

    forget_pre, next_vals = None, None
    for c in range(CHUNKS):
        piece = nexts[:, cut(c)]
        a, b = dot(piece, wf[cut(c), :]), dot(piece, wv[cut(c), :])
        forget_pre = a if c == 0 else forget_pre + a
        next_vals = b if c == 0 else next_vals + b
    next_flow = leak_row * jax.nn.sigmoid(-forget_pre)
    queries = query[...].astype(F32)
    through = by_head(queries * (1.0 - next_flow))
    direct = jnp.sum(by_head(queries * next_flow), axis=1, keepdims=True) * by_head(
        next_vals.astype(BF16).astype(F32)
    )

    r2_copies = []
    for s in range(seqs):
        r1_copies[2 * s].wait_recv()
        q2[s] = ys[second[s], s] + r1[s, 1]
        copy = remote(q2.at[s], r2.at[s], r2_send.at[s], r2_recv.at[s], at(z, second[s]))
        copy.start()
        r2_copies.append(copy)

    for p in z_peers:
        remote(zt.at[p], zt.at[p], zt_send.at[0], zt_recv.at[p], at(p, y)).wait_recv()
    running = jnp.zeros_like(through)
    later_z = jnp.zeros_like(through)
    for j in reversed(range(nz)):
        cols_src[j * seqs * heads:(j + 1) * seqs * heads, :] = jnp.exp(running)
        later_z = jnp.where(z == j, running, later_z)
        running = running + zt[j]
    weights = through * jnp.exp(later_z)
    high, low = halves(weights)
    packed[...] = jnp.concatenate([jnp.concatenate([high, low], axis=0)] * 2, axis=1)
    units = seqs * heads
    parts = [None] * units
    for s in range(seqs):
        got = dot(packed[...], split[s])
        for h in range(heads):
            u = h * seqs + s
            lanes = slice(h * DK, (h + 1) * DK)
            parts[u] = got[u:u + 1, lanes] + got[units + u:units + u + 1, lanes]
    yr[y] = jnp.concatenate(parts, axis=0)
    yr_copies = [
        remote(yr.at[y], yr.at[y], yr_send.at[i], yr_recv.at[y], at(z, p)) for i, p in enumerate(y_peers)
    ]
    for copy in yr_copies:
        copy.start()

    zr_copies = []
    for s in range(seqs):
        r1_copies[2 * s + 1].wait_recv()
        r2_copies[s].wait_recv()
        zs[s] = ys[y, s] + r1[s, 0] + r2[s]
        for i, p in enumerate(z_peers):
            copy = remote(zs.at[s, p], zr.at[z, s], zr_send.at[s, i], zr_recv.at[z, s], at(p, y))
            copy.start()
            zr_copies.append(copy)
        zr[z, s] = zs[s, z]

    for p in y_peers:
        remote(yr.at[p], yr.at[p], yr_send.at[0], yr_recv.at[p], at(z, p)).wait_recv()
    rz[z] = (yr[0] + yr[1]) + (yr[2] + yr[3])
    rz_copies = [
        remote(rz.at[z], rz.at[z], rz_send.at[i], rz_recv.at[z], at(p, y)) for i, p in enumerate(z_peers)
    ]
    for copy in rz_copies:
        copy.start()

    own = DK // (NY * nz)
    cols[...] = jnp.transpose(cols_src[...])
    mine = cols[pl.ds(me * own, own), :]

    def column(j, s):
        one = [
            jnp.broadcast_to(mine[:, c:c + 1], (own, DV))
            for c in (j * units + h * seqs + s for h in range(heads))
        ]
        return jnp.concatenate(one, axis=0)

    scale = [[column(j, s) for s in range(seqs)] for j in range(nz)]
    for p in z_peers:
        for s in range(seqs):
            remote(zr.at[p, s], zr.at[p, s], zr_send.at[0, 0], zr_recv.at[p, s], at(p, y)).wait_recv()
    for s in range(seqs):
        total = scale[0][s] * zr[0, s]
        for j in range(1, nz):
            total = total + scale[j][s] * zr[j, s]
        cache_out[s] = total.astype(BF16)

    for p in z_peers:
        remote(rz.at[p], rz.at[p], rz_send.at[0], rz_recv.at[p], at(p, y)).wait_recv()
    raw = direct
    for j in range(nz):
        raw = raw + rz[j]
    gain_row = gain[...]
    gains = jnp.concatenate(
        [jnp.broadcast_to(gain_row[:, h * DV:(h + 1) * DV], (seqs, DV)) for h in range(heads)], axis=0
    )
    normed = raw * lax.rsqrt(jnp.mean(raw * raw, axis=1, keepdims=True) + EPS) * gains
    read_out[...] = jnp.concatenate(
        [normed[h * seqs:(h + 1) * seqs, :] for h in range(heads)], axis=1
    ).astype(BF16)

    for copy in yt_copies + zt_copies + r1_copies + r2_copies + zr_copies + yr_copies + rz_copies:
        copy.wait_send()


def local(prompt, forget_weight, value_weight, leak, query, next_input, read_gain):
    seqs, span, depth = prompt.shape
    width = forget_weight.shape[1]
    heads = width // DK
    nz = lax.axis_size("sp") // NY
    own = DK // (NY * nz)
    units = seqs * heads
    dma = pltpu.SemaphoreType.DMA
    anywhere = pl.BlockSpec(memory_space=pl.ANY)
    cache, read = pl.pallas_call(
        functools.partial(kernel, nz),
        out_shape=(
            jax.ShapeDtypeStruct((seqs, heads * own, DV), BF16),
            jax.ShapeDtypeStruct((seqs, width), BF16),
        ),
        in_specs=[anywhere] * 7,
        out_specs=(pl.BlockSpec(memory_space=pltpu.VMEM), pl.BlockSpec(memory_space=pltpu.VMEM)),
        scratch_shapes=[
            pltpu.VMEM((seqs * span, depth), BF16),
            pltpu.VMEM((depth, width), BF16),
            pltpu.VMEM((depth, width), BF16),
            pltpu.VMEM((1, width), F32),
            pltpu.VMEM((seqs, width), BF16),
            pltpu.VMEM((seqs, depth), BF16),
            pltpu.VMEM((1, width), F32),
            pltpu.VMEM((seqs * span, width), F32),
            pltpu.VMEM((seqs * span, width), F32),
            pltpu.VMEM((seqs, 2 * span, width), BF16),
            pltpu.VMEM((seqs * span, width), BF16),
            pltpu.VMEM((2 * units, 2 * DK), BF16),
            pltpu.VMEM((NY, seqs, nz, heads * own, DV), F32),
            pltpu.VMEM((seqs, 2 * DK, width), BF16),
            pltpu.VMEM((seqs, 2, nz, heads * own, DV), F32),
            pltpu.VMEM((seqs, nz, heads * own, DV), F32),
            pltpu.VMEM((seqs, nz, heads * own, DV), F32),
            pltpu.VMEM((seqs, nz, heads * own, DV), F32),
            pltpu.VMEM((nz, seqs, heads * own, DV), F32),
            pltpu.VMEM((NY, units, DK), F32),
            pltpu.VMEM((nz, units, DK), F32),
            pltpu.VMEM((NY, units, DV), F32),
            pltpu.VMEM((nz, units, DV), F32),
            pltpu.VMEM((DK, nz * units), F32),
            pltpu.VMEM((nz * units, DK), F32),
            dma((CHUNKS,)),
            dma((CHUNKS,)),
            dma((CHUNKS,)),
            dma((4,)),
            dma((NY - 1,)),
            dma((NY,)),
            dma((nz - 1,)),
            dma((nz,)),
            dma((seqs, 2)),
            dma((seqs, 2)),
            dma((seqs,)),
            dma((seqs,)),
            dma((seqs, nz - 1)),
            dma((nz, seqs)),
            dma((NY - 1,)),
            dma((NY,)),
            dma((nz - 1,)),
            dma((nz,)),
        ],
        compiler_params=pltpu.CompilerParams(
            collective_id=0, has_side_effects=True, vmem_limit_bytes=60 * 1024 * 1024
        ),
    )(
        prompt.reshape(seqs * span, depth),
        forget_weight,
        value_weight,
        leak.reshape(1, width),
        query,
        next_input,
        read_gain.reshape(1, width),
    )
    return cache.reshape(seqs, heads, own, DV), read


def solution(mesh):
    placed = (
        P("gr", "sp", None),
        P(None, "tp"),
        P(None, "tp"),
        P("tp"),
        P("gr", "tp"),
        P("gr", None),
        P("tp"),
    )
    return jax.shard_map(
        local,
        mesh=mesh,
        in_specs=placed,
        out_specs=(P("gr", "tp", "sp", None), P("gr", "tp")),
        check_vma=False,
    )
```

```python
import functools

import jax
import jax.numpy as jnp
from jax import lax
from jax.experimental import pallas as pl
from jax.experimental.pallas import tpu as pltpu
from jax.sharding import PartitionSpec as P

MESH = pl.DeviceIdType.MESH
F32 = jnp.float32
BF16 = jnp.bfloat16
DK = 128
DV = 128
NY = 4
CHUNKS = 8
EPS = 1e-6


def dot(a, b, contract=((1,), (0,))):
    return lax.dot_general(a, b, (contract, ((), ())), preferred_element_type=F32)


def halves(x):
    high = x.astype(BF16)
    return high, (x - high.astype(F32)).astype(BF16)


def kernel(
    nz, prompt, fw, vw, leak_in, query_in, next_in, gain_in, cache_out, read_out,
    x, w, leak, query, nexts, gain, acc, inflow, decays, packed,
    ys, split, r1, q2, r2, zs, zr, yt, zt, yr, rz, cols, cols_src, near, near_src,
    load_sem, small_sem,
    yt_send, yt_recv, zt_send, zt_recv, r1_send, r1_recv, r2_send, r2_recv,
    zr_send, zr_recv, yr_send, yr_recv, rz_send, rz_recv,
):
    seqs = query.shape[0]
    span = x.shape[0] // seqs
    width = query.shape[1]
    heads = width // DK
    depth = x.shape[1]
    step = depth // CHUNKS
    me = lax.axis_index("sp")
    z = lax.div(me, NY)
    y = lax.rem(me, NY)

    def at(zz, yy):
        return {"sp": zz * NY + yy}

    y_peers = [lax.rem(y + d, NY) for d in range(1, NY)]
    z_peers = [lax.rem(z + d, nz) for d in range(1, nz)]

    barrier = pltpu.get_barrier_semaphore()
    for p in y_peers:
        pl.semaphore_signal(barrier, inc=1, device_id=at(z, p), device_id_type=MESH)
    for p in z_peers:
        pl.semaphore_signal(barrier, inc=1, device_id=at(p, y), device_id_type=MESH)

    def cut(c):
        return pl.ds(c * step, step)

    x_copies = [pltpu.make_async_copy(prompt.at[:, cut(c)], x.at[:, cut(c)], load_sem.at[c]) for c in range(CHUNKS)]
    f_copies = [pltpu.make_async_copy(fw.at[cut(c)], w.at[cut(c), 0:width], load_sem.at[c]) for c in range(CHUNKS)]
    v_copies = [pltpu.make_async_copy(vw.at[cut(c)], w.at[cut(c), width:2 * width], load_sem.at[c]) for c in range(CHUNKS)]
    small = [
        pltpu.make_async_copy(src, dst, small_sem.at[i])
        for i, (src, dst) in enumerate(((leak_in, leak), (query_in, query), (next_in, nexts), (gain_in, gain)))
    ]
    for c in range(CHUNKS):
        f_copies[c].start()
        x_copies[c].start()
        v_copies[c].start()
    for copy in small:
        copy.start()

    def remote(src, dst, send, recv, to):
        return pltpu.make_async_remote_copy(
            src_ref=src, dst_ref=dst, send_sem=send, recv_sem=recv, device_id=to, device_id_type=MESH
        )

    def arrive(ref, sem):
        pltpu.make_async_copy(ref, ref, sem).wait()

    for c in range(CHUNKS):
        arrive(w.at[0:2 * step], load_sem.at[c])
        part = dot(x[:, cut(c)], w[cut(c), :])
        if c == 0:
            acc[...] = part
        else:
            acc[...] += part
    for copy in small:
        copy.wait()

    leak_row = leak[...]
    totals = []
    for s in range(seqs):
        rows = pl.ds(s * span, span)
        flow = leak_row * jax.nn.sigmoid(-acc[rows, 0:width])
        inflow[rows, :] = flow
        log = jnp.log(1.0 - flow)
        high, low = halves(log)
        decays[s, 0:span, :] = high
        decays[s, span:2 * span, :] = low
        totals.append(jnp.sum(log, axis=0, keepdims=True))

    def by_head(rows):
        return jnp.concatenate([rows[:, h * DK:(h + 1) * DK] for h in range(heads)], axis=0)

    yt[y] = by_head(jnp.concatenate(totals, axis=0))
    pl.semaphore_wait(barrier, NY - 1 + nz - 1)
    yt_copies = [
        remote(yt.at[y], yt.at[y], yt_send, yt_recv, at(z, p)) for i, p in enumerate(y_peers)
    ]
    for copy in yt_copies:
        copy.start()

    rows_at = lax.broadcasted_iota(jnp.int32, (span, 2 * span), 0)
    cols_at = lax.rem(lax.broadcasted_iota(jnp.int32, (span, 2 * span), 1), span)
    own = DK // (NY * nz)
    upper = jnp.where(cols_at > rows_at, 1.0, 0.0).astype(BF16)

    pair = y + 1 - 2 * lax.rem(y, 2)
    across = NY - 1 - y
    first, second = [], []
    for s in range(seqs):
        first.append(pair if s % 2 == 0 else across)
        second.append(across if s % 2 == 0 else pair)

    far_copies, near_copies = [], []
    for s in range(seqs):
        rows = pl.ds(s * span, span)
        left = dot(upper, decays[s])
        vals = acc[rows, width:2 * width].astype(BF16)
        weighted = (inflow[rows, :] * jnp.exp(left)).astype(BF16)
        for h in range(heads):
            lanes = slice(h * DK, (h + 1) * DK)
            state = dot(weighted[:, lanes], vals[:, lanes], ((0,), (0,)))
            high, low = halves(state)
            split[s, 0:DK, lanes] = high
            split[s, DK:2 * DK, lanes] = low
            for zz in range(nz):
                for yy in range(NY):
                    k = (zz * NY + yy) * own
                    ys[yy, s, zz, h * own:(h + 1) * own, :] = state[k:k + own, :]
        p = first[s]
        beyond = NY - 1 - p if s % 2 == 0 else p + 1 - 2 * lax.rem(p, 2)
        copy = remote(ys.at[beyond, s], r1.at[s, 1], r1_send, r1_recv.at[s, 1], at(z, p))
        copy.start()
        far_copies.append(copy)
    for s in range(seqs):
        p = first[s]
        copy = remote(ys.at[p, s], r1.at[s, 0], r1_send, r1_recv.at[s, 0], at(z, p))
        copy.start()
        near_copies.append(copy)

    for c in range(CHUNKS):
        part = dot(nexts[:, cut(c)], w[cut(c), :])
        next_pre = part if c == 0 else next_pre + part
    forget_pre, next_vals = next_pre[:, 0:width], next_pre[:, width:2 * width]
    next_flow = leak_row * jax.nn.sigmoid(-forget_pre)
    queries = query[...].astype(F32)
    through = by_head(queries * (1.0 - next_flow))
    direct = jnp.sum(by_head(queries * next_flow), axis=1, keepdims=True) * by_head(
        next_vals.astype(BF16).astype(F32)
    )

    arrive(yt.at[0:NY - 1], yt_recv)
    all_y = [yt[j] for j in range(NY)]
    zt[z] = sum(all_y[1:], all_y[0])
    zt_copies = [
        remote(zt.at[z], zt.at[z], zt_send, zt_recv.at[z], at(p, y)) for i, p in enumerate(z_peers)
    ]
    for copy in zt_copies:
        copy.start()

    def after(p):
        return jnp.exp(sum(jnp.where(p < j, all_y[j], 0.0) for j in range(1, NY)))

    units = seqs * heads
    here = after(y)
    near_src[0:units, :] = here
    near_src[units:2 * units, :] = after(pair)
    near_src[2 * units:3 * units, :] = after(across)
    near_src[3 * units:4 * units, :] = jnp.zeros_like(here)
    near[...] = jnp.transpose(near_src[...])

    def spread(rows, lanes):
        return jnp.concatenate([jnp.broadcast_to(rows[:, c:c + 1], (own, DV)) for c in lanes], axis=0)

    def near_scale(target, which, s):
        return [
            spread(near[pl.ds((j * NY + target) * own, own), :], [which * units + h * seqs + s for h in range(heads)])
            for j in range(nz)
        ]

    r2_copies = []
    for s in range(seqs):
        mine, theirs = near_scale(second[s], 0, s), near_scale(second[s], 1 + s % 2, s)
        far_copies[s].wait_recv()
        for j in range(nz):
            q2[s, j] = mine[j] * ys[second[s], s, j] + theirs[j] * r1[s, 1, j]
        copy = remote(q2.at[s], r2.at[s], r2_send, r2_recv.at[s], at(z, second[s]))
        copy.start()
        r2_copies.append(copy)

    zr_copies = []
    for s in range(seqs):
        mine, theirs = near_scale(y, 0, s), near_scale(y, 1 + s % 2, s)
        near_copies[s].wait_recv()
        r2_copies[s].wait_recv()
        for j in range(nz):
            zs[s, j] = (mine[j] * ys[y, s, j] + theirs[j] * r1[s, 0, j]) + r2[s, j]
        for i, p in enumerate(z_peers):
            copy = remote(zs.at[s, p], zr.at[z, s], zr_send, zr_recv.at[s], at(p, y))
            copy.start()
            zr_copies.append(copy)
        zr[z, s] = zs[s, z]

    def add_later(j, total):
        arrive(zt.at[j], zt_recv.at[j])
        return total + zt[j]

    later_z = lax.fori_loop(z + 1, nz, add_later, jnp.zeros_like(through))
    weights = through * here * jnp.exp(later_z)
    high, low = halves(weights)
    packed[...] = jnp.concatenate([jnp.concatenate([high, low], axis=0)] * 2, axis=1)
    parts = [None] * units
    for s in range(seqs):
        got = dot(packed[...], split[s])
        for h in range(heads):
            u = h * seqs + s
            lanes = slice(h * DK, (h + 1) * DK)
            parts[u] = got[u:u + 1, lanes] + got[units + u:units + u + 1, lanes]
    yr[y] = jnp.concatenate(parts, axis=0)
    yr_copies = [
        remote(yr.at[y], yr.at[y], yr_send, yr_recv, at(z, p)) for i, p in enumerate(y_peers)
    ]
    for copy in yr_copies:
        copy.start()

    arrive(yr.at[0:NY - 1], yr_recv)
    rz[z] = (yr[0] + yr[1]) + (yr[2] + yr[3])
    rz_copies = [
        remote(rz.at[z], rz.at[z], rz_send, rz_recv, at(p, y)) for i, p in enumerate(z_peers)
    ]
    for copy in rz_copies:
        copy.start()

    def await_rest(j, carry):
        arrive(zt.at[j], zt_recv.at[j])
        return carry

    lax.fori_loop(0, z, await_rest, 0)
    running = jnp.zeros_like(through)
    for j in reversed(range(nz)):
        cols_src[j * units:(j + 1) * units, :] = jnp.exp(running)
        running = running + zt[j]
    cols[...] = jnp.transpose(cols_src[...])
    mine = cols[pl.ds(me * own, own), :]

    def column(j, s):
        return spread(mine, [j * units + h * seqs + s for h in range(heads)])

    scale = [[column(j, s) for s in range(seqs)] for j in range(nz)]
    for s in range(seqs):
        arrive(zr.at[0:nz - 1, s], zr_recv.at[s])
    for s in range(seqs):
        total = scale[0][s] * zr[0, s]
        for j in range(1, nz):
            total = total + scale[j][s] * zr[j, s]
        cache_out[s] = total.astype(BF16)

    arrive(rz.at[0:nz - 1], rz_recv)
    raw = direct
    for j in range(nz):
        raw = raw + rz[j]
    gain_row = gain[...]
    gains = jnp.concatenate(
        [jnp.broadcast_to(gain_row[:, h * DV:(h + 1) * DV], (seqs, DV)) for h in range(heads)], axis=0
    )
    normed = raw * lax.rsqrt(jnp.mean(raw * raw, axis=1, keepdims=True) + EPS) * gains
    read_out[...] = jnp.concatenate(
        [normed[h * seqs:(h + 1) * seqs, :] for h in range(heads)], axis=1
    ).astype(BF16)

    arrive(yt.at[0:NY - 1], yt_send)
    arrive(zt.at[0:nz - 1], zt_send)
    for i in range(2):
        arrive(r1.at[:, i], r1_send)
    arrive(r2, r2_send)
    arrive(zr.at[0:nz - 1], zr_send)
    arrive(yr.at[0:NY - 1], yr_send)
    arrive(rz.at[0:nz - 1], rz_send)


def local(prompt, forget_weight, value_weight, leak, query, next_input, read_gain):
    seqs, span, depth = prompt.shape
    width = forget_weight.shape[1]
    heads = width // DK
    nz = lax.axis_size("sp") // NY
    own = DK // (NY * nz)
    units = seqs * heads
    dma = pltpu.SemaphoreType.DMA
    anywhere = pl.BlockSpec(memory_space=pl.ANY)
    cache, read = pl.pallas_call(
        functools.partial(kernel, nz),
        out_shape=(
            pltpu.VMEM((seqs, heads * own, DV), BF16),
            pltpu.VMEM((seqs, width), BF16),
        ),
        in_specs=[anywhere] * 7,
        out_specs=(pl.BlockSpec(memory_space=pltpu.VMEM), pl.BlockSpec(memory_space=pltpu.VMEM)),
        scratch_shapes=[
            pltpu.VMEM((seqs * span, depth), BF16),
            pltpu.VMEM((depth, 2 * width), BF16),
            pltpu.VMEM((1, width), F32),
            pltpu.VMEM((seqs, width), BF16),
            pltpu.VMEM((seqs, depth), BF16),
            pltpu.VMEM((1, width), F32),
            pltpu.VMEM((seqs * span, 2 * width), F32),
            pltpu.VMEM((seqs * span, width), F32),
            pltpu.VMEM((seqs, 2 * span, width), BF16),
            pltpu.VMEM((2 * units, 2 * DK), BF16),
            pltpu.VMEM((NY, seqs, nz, heads * own, DV), F32),
            pltpu.VMEM((seqs, 2 * DK, width), BF16),
            pltpu.VMEM((seqs, 2, nz, heads * own, DV), F32),
            pltpu.VMEM((seqs, nz, heads * own, DV), F32),
            pltpu.VMEM((seqs, nz, heads * own, DV), F32),
            pltpu.VMEM((seqs, nz, heads * own, DV), F32),
            pltpu.VMEM((nz, seqs, heads * own, DV), F32),
            pltpu.VMEM((NY, units, DK), F32),
            pltpu.VMEM((nz, units, DK), F32),
            pltpu.VMEM((NY, units, DV), F32),
            pltpu.VMEM((nz, units, DV), F32),
            pltpu.VMEM((DK, nz * units), F32),
            pltpu.VMEM((nz * units, DK), F32),
            pltpu.VMEM((DK, 4 * units), F32),
            pltpu.VMEM((4 * units, DK), F32),
            dma((CHUNKS,)),
            dma((4,)),
            dma,
            dma,
            dma,
            dma((nz,)),
            dma,
            dma((seqs, 2)),
            dma,
            dma((seqs,)),
            dma,
            dma((seqs,)),
            dma,
            dma,
            dma,
            dma,
        ],
        compiler_params=pltpu.CompilerParams(
            collective_id=0, has_side_effects=True, vmem_limit_bytes=60 * 1024 * 1024
        ),
    )(
        prompt.reshape(seqs * span, depth),
        forget_weight,
        value_weight,
        leak.reshape(1, width),
        query,
        next_input,
        read_gain.reshape(1, width),
    )
    return cache.reshape(seqs, heads, own, DV), read


def solution(mesh):
    placed = (
        P("gr", "sp", None),
        P(None, "tp"),
        P(None, "tp"),
        P("tp"),
        P("gr", "tp"),
        P("gr", None),
        P("tp"),
    )
    return jax.shard_map(
        local,
        mesh=mesh,
        in_specs=placed,
        out_specs=(P("gr", "tp", "sp", None), P("gr", "tp")),
        check_vma=False,
    )
```

```python
import functools

import jax
import jax.numpy as jnp
from jax import lax
from jax.experimental import pallas as pl
from jax.experimental.pallas import tpu as pltpu
from jax.sharding import PartitionSpec as P

MESH = pl.DeviceIdType.MESH
F32 = jnp.float32
BF16 = jnp.bfloat16
DK = 128
DV = 128
NY = 4
CHUNKS = 8
EPS = 1e-6


def dot(a, b, contract=((1,), (0,))):
    return lax.dot_general(a, b, (contract, ((), ())), preferred_element_type=F32)


def halves(x):
    high = x.astype(BF16)
    return high, (x - high.astype(F32)).astype(BF16)


def kernel(
    nz, prompt, fw, vw, leak_in, query_in, next_in, gain_in, cache_out, read_out,
    x, w, leak, query, nexts, gain, acc, inflow, decays, packed,
    ys, split, r1, q2, r2, zs, zr, yt, zt, yr, rz, cols, cols_src, near, near_src,
    load_sem, small_sem, corner_in,
    yt_send, yt_recv, zt_send, zt_recv, r1_send, r1_recv, r2_send, r2_recv,
    zr_send, zr_recv, yr_send, yr_recv, rz_send, rz_recv,
):
    seqs = query.shape[0]
    span = x.shape[0] // seqs
    width = query.shape[1]
    heads = width // DK
    depth = x.shape[1]
    step = depth // CHUNKS
    me = lax.axis_index("sp")
    z = lax.div(me, NY)
    y = lax.rem(me, NY)

    def at(zz, yy):
        return {"sp": zz * NY + yy}

    y_peers = [lax.rem(y + d, NY) for d in range(1, NY)]
    z_peers = [1 + lax.rem(z + i - 1, nz - 1) for i in range(1, nz - 1)]
    z_peers.append((nz - 1) * lax.div(nz - z, nz))

    barrier = pltpu.get_barrier_semaphore()
    for p in y_peers:
        pl.semaphore_signal(barrier, inc=1, device_id=at(z, p), device_id_type=MESH)

    @pl.when(me > 0)
    def _():
        for p in z_peers:
            pl.semaphore_signal(barrier, inc=1, device_id=at(p, y), device_id_type=MESH)

    def cut(c):
        return pl.ds(c * step, step)

    x_copies = [pltpu.make_async_copy(prompt.at[:, cut(c)], x.at[:, cut(c)], load_sem.at[c]) for c in range(CHUNKS)]
    f_copies = [pltpu.make_async_copy(fw.at[cut(c)], w.at[cut(c), 0:width], load_sem.at[c]) for c in range(CHUNKS)]
    v_copies = [pltpu.make_async_copy(vw.at[cut(c)], w.at[cut(c), width:2 * width], load_sem.at[c]) for c in range(CHUNKS)]
    small = [
        pltpu.make_async_copy(src, dst, small_sem.at[i])
        for i, (src, dst) in enumerate(((leak_in, leak), (query_in, query), (next_in, nexts), (gain_in, gain)))
    ]
    for c in range(CHUNKS):
        f_copies[c].start()
        x_copies[c].start()
        v_copies[c].start()
    for copy in small:
        copy.start()

    def greet_column():
        pl.semaphore_wait(barrier, NY - 1 + nz - 1)
        for p in z_peers:
            pl.semaphore_signal(corner_in, inc=1, device_id=at(p, y), device_id_type=MESH)

    corner = me == 0
    early = corner & (lax.axis_index("gr") == 0) & (lax.axis_index("tp") == 0)
    pl.when(early)(greet_column)

    def remote(src, dst, send, recv, to):
        return pltpu.make_async_remote_copy(
            src_ref=src, dst_ref=dst, send_sem=send, recv_sem=recv, device_id=to, device_id_type=MESH
        )

    def arrive(ref, sem):
        pltpu.make_async_copy(ref, ref, sem).wait()

    for c in range(CHUNKS):
        arrive(w.at[0:2 * step], load_sem.at[c])
        part = dot(x[:, cut(c)], w[cut(c), :])
        if c == 0:
            acc[...] = part
        else:
            acc[...] += part
    for copy in small:
        copy.wait()

    leak_row = leak[...]
    totals = []
    for s in range(seqs):
        rows = pl.ds(s * span, span)
        flow = leak_row * jax.nn.sigmoid(-acc[rows, 0:width])
        inflow[rows, :] = flow
        log = jnp.log(1.0 - flow)
        high, low = halves(log)
        decays[s, 0:span, :] = high
        decays[s, span:2 * span, :] = low
        totals.append(jnp.sum(log, axis=0, keepdims=True))

    def by_head(rows):
        return jnp.concatenate([rows[:, h * DK:(h + 1) * DK] for h in range(heads)], axis=0)

    yt[y] = by_head(jnp.concatenate(totals, axis=0))
    pl.when(corner & jnp.logical_not(early))(greet_column)
    under = (y == 0) & (z > 0)

    @pl.when(under)
    def _():
        pl.semaphore_wait(barrier, NY - 1 + nz - 2)

    @pl.when(y > 0)
    def _():
        pl.semaphore_wait(barrier, NY - 1 + nz - 1)

    yt_copies = [
        remote(yt.at[y], yt.at[y], yt_send, yt_recv, at(z, p)) for i, p in enumerate(y_peers)
    ]
    for copy in yt_copies:
        copy.start()

    rows_at = lax.broadcasted_iota(jnp.int32, (span, 2 * span), 0)
    cols_at = lax.rem(lax.broadcasted_iota(jnp.int32, (span, 2 * span), 1), span)
    own = DK // (NY * nz)
    upper = jnp.where(cols_at > rows_at, 1.0, 0.0).astype(BF16)

    pair = y + 1 - 2 * lax.rem(y, 2)
    across = NY - 1 - y
    first, second = [], []
    for s in range(seqs):
        first.append(pair if s % 2 == 0 else across)
        second.append(across if s % 2 == 0 else pair)

    far_copies, near_copies = [], []
    for s in range(seqs):
        rows = pl.ds(s * span, span)
        left = dot(upper, decays[s])
        vals = acc[rows, width:2 * width].astype(BF16)
        weighted = (inflow[rows, :] * jnp.exp(left)).astype(BF16)
        for h in range(heads):
            lanes = slice(h * DK, (h + 1) * DK)
            state = dot(weighted[:, lanes], vals[:, lanes], ((0,), (0,)))
            high, low = halves(state)
            split[s, 0:DK, lanes] = high
            split[s, DK:2 * DK, lanes] = low
            for zz in range(nz):
                for yy in range(NY):
                    k = (zz * NY + yy) * own
                    ys[yy, s, zz, h * own:(h + 1) * own, :] = state[k:k + own, :]
    for s in range(seqs):
        p = first[s]
        beyond = NY - 1 - p if s % 2 == 0 else p + 1 - 2 * lax.rem(p, 2)
        copy = remote(ys.at[beyond, s], r1.at[s, 1], r1_send, r1_recv.at[s, 1], at(z, p))
        copy.start()
        far_copies.append(copy)
    for s in range(seqs):
        p = first[s]
        copy = remote(ys.at[p, s], r1.at[s, 0], r1_send, r1_recv.at[s, 0], at(z, p))
        copy.start()
        near_copies.append(copy)

    for c in range(CHUNKS):
        part = dot(nexts[:, cut(c)], w[cut(c), :])
        next_pre = part if c == 0 else next_pre + part
    forget_pre, next_vals = next_pre[:, 0:width], next_pre[:, width:2 * width]
    next_flow = leak_row * jax.nn.sigmoid(-forget_pre)
    queries = query[...].astype(F32)
    through = by_head(queries * (1.0 - next_flow))
    direct = jnp.sum(by_head(queries * next_flow), axis=1, keepdims=True) * by_head(
        next_vals.astype(BF16).astype(F32)
    )

    arrive(yt.at[0:NY - 1], yt_recv)
    all_y = [yt[j] for j in range(NY)]
    zt[z] = sum(all_y[1:], all_y[0])
    zt_copies = [
        remote(zt.at[z], zt.at[z], zt_send, zt_recv.at[z], at(p, y)) for i, p in enumerate(z_peers)
    ]
    for copy in zt_copies[:-1]:
        copy.start()

    @pl.when(under)
    def _():
        pl.semaphore_wait(corner_in, 1)

    zt_copies[-1].start()

    def after(p):
        return jnp.exp(sum(jnp.where(p < j, all_y[j], 0.0) for j in range(1, NY)))

    units = seqs * heads
    here = after(y)
    near_src[0:units, :] = here
    near_src[units:2 * units, :] = after(pair)
    near_src[2 * units:3 * units, :] = after(across)
    near_src[3 * units:4 * units, :] = jnp.zeros_like(here)
    near[...] = jnp.transpose(near_src[...])

    def spread(rows, lanes):
        return jnp.concatenate([jnp.broadcast_to(rows[:, c:c + 1], (own, DV)) for c in lanes], axis=0)

    def near_scale(target, which, s):
        return [
            spread(near[pl.ds((j * NY + target) * own, own), :], [which * units + h * seqs + s for h in range(heads)])
            for j in range(nz)
        ]

    def read_segments():
        def add_later(j, total):
            arrive(zt.at[j], zt_recv.at[j])
            return total + zt[j]

        later_z = lax.fori_loop(z + 1, nz, add_later, jnp.zeros_like(through))
        weights = through * here * jnp.exp(later_z)
        high, low = halves(weights)
        packed[...] = jnp.concatenate([jnp.concatenate([high, low], axis=0)] * 2, axis=1)
        parts = [None] * units
        for s in range(seqs):
            got = dot(packed[...], split[s])
            for h in range(heads):
                u = h * seqs + s
                lanes = slice(h * DK, (h + 1) * DK)
                parts[u] = got[u:u + 1, lanes] + got[units + u:units + u + 1, lanes]
        yr[y] = jnp.concatenate(parts, axis=0)
        yr_copies = [
            remote(yr.at[y], yr.at[y], yr_send, yr_recv, at(z, p)) for i, p in enumerate(y_peers)
        ]
        for copy in yr_copies:
            copy.start()


    def share_read():
        arrive(yr.at[0:NY - 1], yr_recv)
        rz[z] = (yr[0] + yr[1]) + (yr[2] + yr[3])
        rz_copies = [
            remote(rz.at[z], rz.at[z], rz_send, rz_recv, at(p, y)) for i, p in enumerate(z_peers)
        ]
        for copy in rz_copies:
            copy.start()


    top, bottom = z == nz - 1, z == 0
    pl.when(top)(read_segments)

    r2_copies = []
    for s in range(seqs):
        mine, theirs = near_scale(second[s], 0, s), near_scale(second[s], 1 + s % 2, s)
        far_copies[s].wait_recv()
        for j in range(nz):
            q2[s, j] = mine[j] * ys[second[s], s, j] + theirs[j] * r1[s, 1, j]
        copy = remote(q2.at[s], r2.at[s], r2_send, r2_recv.at[s], at(z, second[s]))
        copy.start()
        r2_copies.append(copy)

    pl.when(bottom)(read_segments)
    pl.when(top)(share_read)

    zr_copies = []
    for s in range(seqs):
        mine, theirs = near_scale(y, 0, s), near_scale(y, 1 + s % 2, s)
        near_copies[s].wait_recv()
        r2_copies[s].wait_recv()
        for j in range(nz):
            zs[s, j] = (mine[j] * ys[y, s, j] + theirs[j] * r1[s, 0, j]) + r2[s, j]
        for i, p in enumerate(z_peers):
            copy = remote(zs.at[s, p], zr.at[z, s], zr_send, zr_recv.at[s], at(p, y))
            copy.start()
            zr_copies.append(copy)
        zr[z, s] = zs[s, z]

    pl.when(jnp.logical_not(top | bottom))(read_segments)
    pl.when(jnp.logical_not(top))(share_read)

    def await_rest(j, carry):
        arrive(zt.at[j], zt_recv.at[j])
        return carry

    lax.fori_loop(0, z, await_rest, 0)
    running = jnp.zeros_like(through)
    for j in reversed(range(nz)):
        cols_src[j * units:(j + 1) * units, :] = jnp.exp(running)
        running = running + zt[j]
    cols[...] = jnp.transpose(cols_src[...])
    mine = cols[pl.ds(me * own, own), :]

    def column(j, s):
        return spread(mine, [j * units + h * seqs + s for h in range(heads)])

    scale = [[column(j, s) for s in range(seqs)] for j in range(nz)]
    for s in range(seqs):
        arrive(zr.at[0:nz - 1, s], zr_recv.at[s])
    for s in range(seqs):
        total = scale[0][s] * zr[0, s]
        for j in range(1, nz):
            total = total + scale[j][s] * zr[j, s]
        cache_out[s] = total.astype(BF16)

    arrive(rz.at[0:nz - 1], rz_recv)
    raw = direct
    for j in range(nz):
        raw = raw + rz[j]
    gain_row = gain[...]
    gains = jnp.concatenate(
        [jnp.broadcast_to(gain_row[:, h * DV:(h + 1) * DV], (seqs, DV)) for h in range(heads)], axis=0
    )
    normed = raw * lax.rsqrt(jnp.mean(raw * raw, axis=1, keepdims=True) + EPS) * gains
    read_out[...] = jnp.concatenate(
        [normed[h * seqs:(h + 1) * seqs, :] for h in range(heads)], axis=1
    ).astype(BF16)

    arrive(yt.at[0:NY - 1], yt_send)
    arrive(zt.at[0:nz - 1], zt_send)
    for i in range(2):
        arrive(r1.at[:, i], r1_send)
    arrive(r2, r2_send)
    arrive(zr.at[0:nz - 1], zr_send)
    arrive(yr.at[0:NY - 1], yr_send)
    arrive(rz.at[0:nz - 1], rz_send)


def local(prompt, forget_weight, value_weight, leak, query, next_input, read_gain):
    seqs, span, depth = prompt.shape
    width = forget_weight.shape[1]
    heads = width // DK
    nz = lax.axis_size("sp") // NY
    own = DK // (NY * nz)
    units = seqs * heads
    dma = pltpu.SemaphoreType.DMA
    anywhere = pl.BlockSpec(memory_space=pl.ANY)
    cache, read = pl.pallas_call(
        functools.partial(kernel, nz),
        out_shape=(
            pltpu.VMEM((seqs, heads * own, DV), BF16),
            pltpu.VMEM((seqs, width), BF16),
        ),
        in_specs=[anywhere] * 7,
        out_specs=(pl.BlockSpec(memory_space=pltpu.VMEM), pl.BlockSpec(memory_space=pltpu.VMEM)),
        scratch_shapes=[
            pltpu.VMEM((seqs * span, depth), BF16),
            pltpu.VMEM((depth, 2 * width), BF16),
            pltpu.VMEM((1, width), F32),
            pltpu.VMEM((seqs, width), BF16),
            pltpu.VMEM((seqs, depth), BF16),
            pltpu.VMEM((1, width), F32),
            pltpu.VMEM((seqs * span, 2 * width), F32),
            pltpu.VMEM((seqs * span, width), F32),
            pltpu.VMEM((seqs, 2 * span, width), BF16),
            pltpu.VMEM((2 * units, 2 * DK), BF16),
            pltpu.VMEM((NY, seqs, nz, heads * own, DV), F32),
            pltpu.VMEM((seqs, 2 * DK, width), BF16),
            pltpu.VMEM((seqs, 2, nz, heads * own, DV), F32),
            pltpu.VMEM((seqs, nz, heads * own, DV), F32),
            pltpu.VMEM((seqs, nz, heads * own, DV), F32),
            pltpu.VMEM((seqs, nz, heads * own, DV), F32),
            pltpu.VMEM((nz, seqs, heads * own, DV), F32),
            pltpu.VMEM((NY, units, DK), F32),
            pltpu.VMEM((nz, units, DK), F32),
            pltpu.VMEM((NY, units, DV), F32),
            pltpu.VMEM((nz, units, DV), F32),
            pltpu.VMEM((DK, nz * units), F32),
            pltpu.VMEM((nz * units, DK), F32),
            pltpu.VMEM((DK, 4 * units), F32),
            pltpu.VMEM((4 * units, DK), F32),
            dma((CHUNKS,)),
            dma((4,)),
            pltpu.SemaphoreType.REGULAR,
            dma,
            dma,
            dma,
            dma((nz,)),
            dma,
            dma((seqs, 2)),
            dma,
            dma((seqs,)),
            dma,
            dma((seqs,)),
            dma,
            dma,
            dma,
            dma,
        ],
        compiler_params=pltpu.CompilerParams(
            collective_id=0, has_side_effects=True, vmem_limit_bytes=60 * 1024 * 1024
        ),
    )(
        prompt.reshape(seqs * span, depth),
        forget_weight,
        value_weight,
        leak.reshape(1, width),
        query,
        next_input,
        read_gain.reshape(1, width),
    )
    return cache.reshape(seqs, heads, own, DV), read


def solution(mesh):
    placed = (
        P("gr", "sp", None),
        P(None, "tp"),
        P(None, "tp"),
        P("tp"),
        P("gr", "tp"),
        P("gr", None),
        P("tp"),
    )
    return jax.shard_map(
        local,
        mesh=mesh,
        in_specs=placed,
        out_specs=(P("gr", "tp", "sp", None), P("gr", "tp")),
        check_vma=False,
    )
```

```python
import functools

import jax
import jax.numpy as jnp
from jax import lax
from jax.experimental import pallas as pl
from jax.experimental.pallas import tpu as pltpu
from jax.sharding import PartitionSpec as P

MESH = pl.DeviceIdType.MESH
F32 = jnp.float32
BF16 = jnp.bfloat16
DK = 128
DV = 128
NY = 4
CHUNKS = 8
EPS = 1e-6


def dot(a, b, contract=((1,), (0,))):
    return lax.dot_general(a, b, (contract, ((), ())), preferred_element_type=F32)


def halves(x):
    high = x.astype(BF16)
    return high, (x - high.astype(F32)).astype(BF16)


def kernel(
    nz, prompt, fw, vw, leak_in, query_in, next_in, gain_in, cache_out, read_out,
    x, w, leak, query, nexts, gain, acc, inflow, decays, packed,
    ys, split, r1, q2, r2, zs, zr, yt, ct, lt, zt, yr, rz, cols, cols_src, near, near_src,
    load_sem, small_sem, corner_in,
    yt_send, yt_recv, ct_send, ct_recv, lt_send, lt_recv, zt_send, zt_recv, r1_send, r1_recv, r2_send, r2_recv,
    zr_send, zr_recv, yr_send, yr_recv, rz_send, rz_recv,
):
    seqs = query.shape[0]
    span = x.shape[0] // seqs
    width = query.shape[1]
    heads = width // DK
    depth = x.shape[1]
    step = depth // CHUNKS
    me = lax.axis_index("sp")
    z = lax.div(me, NY)
    y = lax.rem(me, NY)

    def at(zz, yy):
        return {"sp": zz * NY + yy}

    y_peers = [lax.rem(y + d, NY) for d in range(1, NY)]
    z_peers = [i + lax.div(i - z + nz, nz) for i in range(nz - 1)]

    barrier = pltpu.get_barrier_semaphore()
    for p in y_peers:
        pl.semaphore_signal(barrier, inc=1, device_id=at(z, p), device_id_type=MESH)

    @pl.when(me > 0)
    def _():
        for p in z_peers:
            pl.semaphore_signal(barrier, inc=1, device_id=at(p, y), device_id_type=MESH)

    def cut(c):
        return pl.ds(c * step, step)

    x_copies = [pltpu.make_async_copy(prompt.at[:, cut(c)], x.at[:, cut(c)], load_sem.at[c]) for c in range(CHUNKS)]
    f_copies = [pltpu.make_async_copy(fw.at[cut(c)], w.at[cut(c), 0:width], load_sem.at[c]) for c in range(CHUNKS)]
    v_copies = [pltpu.make_async_copy(vw.at[cut(c)], w.at[cut(c), width:2 * width], load_sem.at[c]) for c in range(CHUNKS)]
    small = [
        pltpu.make_async_copy(src, dst, small_sem.at[i])
        for i, (src, dst) in enumerate(((leak_in, leak), (query_in, query), (next_in, nexts), (gain_in, gain)))
    ]
    for c in range(CHUNKS):
        f_copies[c].start()
        x_copies[c].start()
        v_copies[c].start()
    for copy in small:
        copy.start()

    def greet_column():
        pl.semaphore_wait(barrier, NY - 1 + nz - 1)
        for p in z_peers:
            pl.semaphore_signal(corner_in, inc=1, device_id=at(p, y), device_id_type=MESH)

    corner = me == 0
    early = corner & (lax.axis_index("gr") == 0) & (lax.axis_index("tp") == 0)
    pl.when(early)(greet_column)

    def remote(src, dst, send, recv, to):
        return pltpu.make_async_remote_copy(
            src_ref=src, dst_ref=dst, send_sem=send, recv_sem=recv, device_id=to, device_id_type=MESH
        )

    def arrive(ref, sem):
        pltpu.make_async_copy(ref, ref, sem).wait()

    for c in range(CHUNKS):
        arrive(w.at[0:2 * step], load_sem.at[c])
        part = dot(x[:, cut(c)], w[cut(c), :])
        if c == 0:
            acc[...] = part
        else:
            acc[...] += part
    for copy in small:
        copy.wait()

    leak_row = leak[...]
    totals = []
    for s in range(seqs):
        rows = pl.ds(s * span, span)
        flow = leak_row * jax.nn.sigmoid(-acc[rows, 0:width])
        inflow[rows, :] = flow
        log = jnp.log(1.0 - flow)
        high, low = halves(log)
        decays[s, 0:span, :] = high
        decays[s, span:2 * span, :] = low
        totals.append(jnp.sum(log, axis=0, keepdims=True))

    def by_head(rows):
        return jnp.concatenate([rows[:, h * DK:(h + 1) * DK] for h in range(heads)], axis=0)

    yt[y] = by_head(jnp.concatenate(totals, axis=0))
    pl.when(corner & jnp.logical_not(early))(greet_column)
    under = (y == 0) & (z > 0)

    @pl.when(under)
    def _():
        pl.semaphore_wait(barrier, NY - 1 + nz - 2)

    @pl.when(y > 0)
    def _():
        pl.semaphore_wait(barrier, NY - 1 + nz - 1)

    yt_copies = [
        remote(yt.at[y], yt.at[y], yt_send, yt_recv, at(z, p)) for i, p in enumerate(y_peers)
    ]
    for copy in yt_copies:
        copy.start()
    for j in range(1, nz - 1):
        pl.when(z > j)(remote(yt.at[y], ct.at[z], ct_send, ct_recv.at[z], at(j, y)).start)

    rows_at = lax.broadcasted_iota(jnp.int32, (span, 2 * span), 0)
    cols_at = lax.rem(lax.broadcasted_iota(jnp.int32, (span, 2 * span), 1), span)
    own = DK // (NY * nz)
    upper = jnp.where(cols_at > rows_at, 1.0, 0.0).astype(BF16)

    pair = y + 1 - 2 * lax.rem(y, 2)
    across = NY - 1 - y
    first, second = [], []
    for s in range(seqs):
        first.append(pair if s % 2 == 0 else across)
        second.append(across if s % 2 == 0 else pair)

    far_copies, near_copies = [], []
    for s in range(seqs):
        rows = pl.ds(s * span, span)
        left = dot(upper, decays[s])
        vals = acc[rows, width:2 * width].astype(BF16)
        weighted = (inflow[rows, :] * jnp.exp(left)).astype(BF16)
        for h in range(heads):
            lanes = slice(h * DK, (h + 1) * DK)
            state = dot(weighted[:, lanes], vals[:, lanes], ((0,), (0,)))
            high, low = halves(state)
            split[s, 0:DK, lanes] = high
            split[s, DK:2 * DK, lanes] = low
            for zz in range(nz):
                for yy in range(NY):
                    k = (zz * NY + yy) * own
                    ys[yy, s, zz, h * own:(h + 1) * own, :] = state[k:k + own, :]
    for s in range(seqs):
        p = first[s]
        beyond = NY - 1 - p if s % 2 == 0 else p + 1 - 2 * lax.rem(p, 2)
        copy = remote(ys.at[beyond, s], r1.at[s, 1], r1_send, r1_recv.at[s, 1], at(z, p))
        copy.start()
        far_copies.append(copy)
    for s in range(seqs):
        p = first[s]
        copy = remote(ys.at[p, s], r1.at[s, 0], r1_send, r1_recv.at[s, 0], at(z, p))
        copy.start()
        near_copies.append(copy)

    for c in range(CHUNKS):
        part = dot(nexts[:, cut(c)], w[cut(c), :])
        next_pre = part if c == 0 else next_pre + part
    forget_pre, next_vals = next_pre[:, 0:width], next_pre[:, width:2 * width]
    next_flow = leak_row * jax.nn.sigmoid(-forget_pre)
    queries = query[...].astype(F32)
    through = by_head(queries * (1.0 - next_flow))
    direct = jnp.sum(by_head(queries * next_flow), axis=1, keepdims=True) * by_head(
        next_vals.astype(BF16).astype(F32)
    )

    arrive(yt.at[0:NY - 1], yt_recv)
    all_y = [yt[j] for j in range(NY)]
    zt[z] = sum(all_y[1:], all_y[0])
    zt_copies = [
        remote(zt.at[z], zt.at[z], zt_send, zt_recv.at[z], at(p, y)) for i, p in enumerate(z_peers)
    ]
    pl.when(jnp.logical_not(under))(zt_copies[0].start)
    for copy in zt_copies[1:]:
        copy.start()

    @pl.when(under)
    def _():
        pl.semaphore_wait(corner_in, 1)
        zt_copies[0].start()


    def after(p):
        return jnp.exp(sum(jnp.where(p < j, all_y[j], 0.0) for j in range(1, NY)))

    units = seqs * heads
    here = after(y)
    near_src[0:units, :] = here
    near_src[units:2 * units, :] = after(pair)
    near_src[2 * units:3 * units, :] = after(across)
    near_src[3 * units:4 * units, :] = jnp.zeros_like(here)
    near[...] = jnp.transpose(near_src[...])

    def spread(rows, lanes):
        return jnp.concatenate([jnp.broadcast_to(rows[:, c:c + 1], (own, DV)) for c in lanes], axis=0)

    def near_scale(target, which, s):
        return [
            spread(near[pl.ds((j * NY + target) * own, own), :], [which * units + h * seqs + s for h in range(heads)])
            for j in range(nz)
        ]

    def read_segments(later_z):
        weights = through * here * jnp.exp(later_z)
        high, low = halves(weights)
        packed[...] = jnp.concatenate([jnp.concatenate([high, low], axis=0)] * 2, axis=1)
        parts = [None] * units
        for s in range(seqs):
            got = dot(packed[...], split[s])
            for h in range(heads):
                u = h * seqs + s
                lanes = slice(h * DK, (h + 1) * DK)
                parts[u] = got[u:u + 1, lanes] + got[units + u:units + u + 1, lanes]
        rz[z] = jnp.concatenate(parts, axis=0)
        for p in z_peers:
            remote(rz.at[z], rz.at[z], rz_send, rz_recv, at(p, y)).start()

    def add_arrived(totals, sems):
        def add(j, total):
            arrive(totals.at[j], sems.at[j])
            return total + totals[j]

        return lax.fori_loop(z + 1, nz, add, jnp.zeros_like(through))

    def share_later():
        lt[y] = add_arrived(ct, ct_recv)
        for p in y_peers:
            remote(lt.at[y], lt.at[y], lt_send, lt_recv, at(z, p)).start()

    top, upper_half, inner = z == nz - 1, z >= nz // 2, (z > 0) & (z < nz - 1)

    @pl.when(top)
    def _():
        read_segments(jnp.zeros_like(through))

    pl.when(inner & upper_half)(share_later)

    r2_copies = []
    for s in range(seqs):
        mine, theirs = near_scale(second[s], 0, s), near_scale(second[s], 1 + s % 2, s)
        far_copies[s].wait_recv()
        for j in range(nz):
            q2[s, j] = mine[j] * ys[second[s], s, j] + theirs[j] * r1[s, 1, j]
        copy = remote(q2.at[s], r2.at[s], r2_send, r2_recv.at[s], at(z, second[s]))
        copy.start()
        r2_copies.append(copy)

    pl.when(inner & jnp.logical_not(upper_half))(share_later)

    @pl.when(inner)
    def _():
        arrive(lt.at[0:NY - 1], lt_recv)
        read_segments((lt[0] + lt[1]) + (lt[2] + lt[3]))

    @pl.when(z == 0)
    def _():
        read_segments(add_arrived(zt, zt_recv))

    for s in range(seqs):
        mine, theirs = near_scale(y, 0, s), near_scale(y, 1 + s % 2, s)
        near_copies[s].wait_recv()
        r2_copies[s].wait_recv()
        for j in range(nz):
            zs[j, s] = (mine[j] * ys[y, s, j] + theirs[j] * r1[s, 0, j]) + r2[s, j]
        zr[z, s] = zs[z, s]

    def send_state(p):
        remote(zs.at[p], zr.at[z], zr_send, zr_recv, at(p, y)).start()

    for p in z_peers:
        send_state(p)

    def await_rest(j, carry):
        arrive(zt.at[j], zt_recv.at[j])
        return carry

    lax.fori_loop(0, z, await_rest, 0)

    @pl.when(z > 0)
    def _():
        lax.fori_loop(z + 1, nz, await_rest, 0)

    running = jnp.zeros_like(through)
    for j in reversed(range(nz)):
        cols_src[j * units:(j + 1) * units, :] = jnp.exp(running)
        running = running + zt[j]
    cols[...] = jnp.transpose(cols_src[...])
    mine = cols[pl.ds(me * own, own), :]

    def column(j, s):
        return spread(mine, [j * units + h * seqs + s for h in range(heads)])

    scale = [[column(j, s) for s in range(seqs)] for j in range(nz)]
    arrive(rz.at[0:nz - 1], rz_recv)
    column_read = rz[0]
    for j in range(1, nz):
        column_read = column_read + rz[j]
    yr[y] = column_read
    for p in y_peers:
        remote(yr.at[y], yr.at[y], yr_send, yr_recv, at(z, p)).start()

    arrive(zr.at[0:nz - 1], zr_recv)
    for s in range(seqs):
        total = scale[0][s] * zr[0, s]
        for j in range(1, nz):
            total = total + scale[j][s] * zr[j, s]
        cache_out[s] = total.astype(BF16)

    arrive(yr.at[0:NY - 1], yr_recv)
    raw = direct + ((yr[0] + yr[1]) + (yr[2] + yr[3]))
    gain_row = gain[...]
    gains = jnp.concatenate(
        [jnp.broadcast_to(gain_row[:, h * DV:(h + 1) * DV], (seqs, DV)) for h in range(heads)], axis=0
    )
    normed = raw * lax.rsqrt(jnp.mean(raw * raw, axis=1, keepdims=True) + EPS) * gains
    read_out[...] = jnp.concatenate(
        [normed[h * seqs:(h + 1) * seqs, :] for h in range(heads)], axis=1
    ).astype(BF16)

    arrive(yt.at[0:NY - 1], yt_send)

    def await_sent(j, carry):
        arrive(ct.at[0], ct_send)
        return carry

    lax.fori_loop(1, z, await_sent, 0)

    @pl.when(inner)
    def _():
        arrive(lt.at[0:NY - 1], lt_send)

    arrive(zt.at[0:nz - 1], zt_send)
    for i in range(2):
        arrive(r1.at[:, i], r1_send)
    arrive(r2, r2_send)
    arrive(zr.at[0:nz - 1], zr_send)
    arrive(yr.at[0:NY - 1], yr_send)
    arrive(rz.at[0:nz - 1], rz_send)


def local(prompt, forget_weight, value_weight, leak, query, next_input, read_gain):
    seqs, span, depth = prompt.shape
    width = forget_weight.shape[1]
    heads = width // DK
    nz = lax.axis_size("sp") // NY
    own = DK // (NY * nz)
    units = seqs * heads
    dma = pltpu.SemaphoreType.DMA
    anywhere = pl.BlockSpec(memory_space=pl.ANY)
    cache, read = pl.pallas_call(
        functools.partial(kernel, nz),
        out_shape=(
            pltpu.VMEM((seqs, heads * own, DV), BF16),
            pltpu.VMEM((seqs, width), BF16),
        ),
        in_specs=[anywhere] * 7,
        out_specs=(pl.BlockSpec(memory_space=pltpu.VMEM), pl.BlockSpec(memory_space=pltpu.VMEM)),
        scratch_shapes=[
            pltpu.VMEM((seqs * span, depth), BF16),
            pltpu.VMEM((depth, 2 * width), BF16),
            pltpu.VMEM((1, width), F32),
            pltpu.VMEM((seqs, width), BF16),
            pltpu.VMEM((seqs, depth), BF16),
            pltpu.VMEM((1, width), F32),
            pltpu.VMEM((seqs * span, 2 * width), F32),
            pltpu.VMEM((seqs * span, width), F32),
            pltpu.VMEM((seqs, 2 * span, width), BF16),
            pltpu.VMEM((2 * units, 2 * DK), BF16),
            pltpu.VMEM((NY, seqs, nz, heads * own, DV), F32),
            pltpu.VMEM((seqs, 2 * DK, width), BF16),
            pltpu.VMEM((seqs, 2, nz, heads * own, DV), F32),
            pltpu.VMEM((seqs, nz, heads * own, DV), F32),
            pltpu.VMEM((seqs, nz, heads * own, DV), F32),
            pltpu.VMEM((nz, seqs, heads * own, DV), F32),
            pltpu.VMEM((nz, seqs, heads * own, DV), F32),
            pltpu.VMEM((NY, units, DK), F32),
            pltpu.VMEM((nz, units, DK), F32),
            pltpu.VMEM((NY, units, DK), F32),
            pltpu.VMEM((nz, units, DK), F32),
            pltpu.VMEM((NY, units, DV), F32),
            pltpu.VMEM((nz, units, DV), F32),
            pltpu.VMEM((DK, nz * units), F32),
            pltpu.VMEM((nz * units, DK), F32),
            pltpu.VMEM((DK, 4 * units), F32),
            pltpu.VMEM((4 * units, DK), F32),
            dma((CHUNKS,)),
            dma((4,)),
            pltpu.SemaphoreType.REGULAR,
            dma,
            dma,
            dma,
            dma((nz,)),
            dma,
            dma,
            dma,
            dma((nz,)),
            dma,
            dma((seqs, 2)),
            dma,
            dma((seqs,)),
            dma,
            dma,
            dma,
            dma,
            dma,
            dma,
        ],
        compiler_params=pltpu.CompilerParams(
            collective_id=0, has_side_effects=True, vmem_limit_bytes=60 * 1024 * 1024
        ),
    )(
        prompt.reshape(seqs * span, depth),
        forget_weight,
        value_weight,
        leak.reshape(1, width),
        query,
        next_input,
        read_gain.reshape(1, width),
    )
    return cache.reshape(seqs, heads, own, DV), read


def solution(mesh):
    placed = (
        P("gr", "sp", None),
        P(None, "tp"),
        P(None, "tp"),
        P("tp"),
        P("gr", "tp"),
        P("gr", None),
        P("tp"),
    )
    return jax.shard_map(
        local,
        mesh=mesh,
        in_specs=placed,
        out_specs=(P("gr", "tp", "sp", None), P("gr", "tp")),
        check_vma=False,
    )
```

```python
import functools

import jax
import jax.numpy as jnp
from jax import lax
from jax.experimental import pallas as pl
from jax.experimental.pallas import tpu as pltpu
from jax.sharding import PartitionSpec as P

MESH = pl.DeviceIdType.MESH
F32 = jnp.float32
BF16 = jnp.bfloat16
DK = 128
DV = 128
NY = 4
CHUNKS = 8
EPS = 1e-6


def dot(a, b, contract=((1,), (0,))):
    return lax.dot_general(a, b, (contract, ((), ())), preferred_element_type=F32)


def halves(x):
    high = x.astype(BF16)
    return high, (x - high.astype(F32)).astype(BF16)


def kernel(
    nz, prompt, fw, vw, leak_in, query_in, next_in, gain_in, cache_out, read_out,
    x, w, leak, query, nexts, gain, acc, inflow, decays, packed,
    ys, split, r1, q2, r2, zs, zr, yt, ct, lt, zt, yr, rz, cols, cols_src, near, near_src,
    load_sem, small_sem, corner_in,
    sent, yt_recv, ct_recv, lt_recv, zt_recv, r1_recv, r2_recv, zr_recv, yr_recv, rz_recv,
):
    seqs = query.shape[0]
    span = x.shape[0] // seqs
    width = query.shape[1]
    heads = width // DK
    depth = x.shape[1]
    step = depth // CHUNKS
    me = lax.axis_index("sp")
    z = lax.div(me, NY)
    y = lax.rem(me, NY)

    def at(zz, yy):
        return {"sp": zz * NY + yy}

    y_peers = [lax.rem(y + d, NY) for d in range(1, NY)]
    z_peers = [i + lax.div(i - z + nz, nz) for i in range(nz - 1)]

    def cut(c):
        return pl.ds(c * step, step)

    x_copies = [pltpu.make_async_copy(prompt.at[:, cut(c)], x.at[:, cut(c)], load_sem.at[c]) for c in range(CHUNKS)]
    f_copies = [pltpu.make_async_copy(fw.at[cut(c)], w.at[cut(c), 0:width], load_sem.at[c]) for c in range(CHUNKS)]
    v_copies = [pltpu.make_async_copy(vw.at[cut(c)], w.at[cut(c), width:2 * width], load_sem.at[c]) for c in range(CHUNKS)]
    small = [
        pltpu.make_async_copy(src, dst, small_sem.at[i])
        for i, (src, dst) in enumerate(((leak_in, leak), (query_in, query), (next_in, nexts), (gain_in, gain)))
    ]
    for c in range(CHUNKS):
        f_copies[c].start()
        x_copies[c].start()
        v_copies[c].start()
    for copy in small:
        copy.start()

    barrier = pltpu.get_barrier_semaphore()
    for p in y_peers:
        pl.semaphore_signal(barrier, inc=1, device_id=at(z, p), device_id_type=MESH)

    @pl.when(me > 0)
    def _():
        for p in z_peers:
            pl.semaphore_signal(barrier, inc=1, device_id=at(p, y), device_id_type=MESH)

    def greet_column():
        pl.semaphore_wait(barrier, NY - 1 + nz - 1)
        for p in z_peers:
            pl.semaphore_signal(corner_in, inc=1, device_id=at(p, y), device_id_type=MESH)

    corner = me == 0
    early = corner & (lax.axis_index("gr") == 0) & (lax.axis_index("tp") == 0)
    pl.when(early)(greet_column)

    def remote(src, dst, send, recv, to):
        return pltpu.make_async_remote_copy(
            src_ref=src, dst_ref=dst, send_sem=send, recv_sem=recv, device_id=to, device_id_type=MESH
        )

    def arrive(ref, sem):
        pltpu.make_async_copy(ref, ref, sem).wait()

    for c in range(CHUNKS):
        arrive(w.at[0:2 * step], load_sem.at[c])
        part = dot(x[:, cut(c)], w[cut(c), :])
        if c == 0:
            acc[...] = part
        else:
            acc[...] += part
    for copy in small:
        copy.wait()

    leak_row = leak[...]
    totals = []
    for s in range(seqs):
        rows = pl.ds(s * span, span)
        flow = leak_row * jax.nn.sigmoid(-acc[rows, 0:width])
        inflow[rows, :] = flow
        log = jnp.log(1.0 - flow)
        high, low = halves(log)
        decays[s, 0:span, :] = high
        decays[s, span:2 * span, :] = low
        totals.append(jnp.sum(log, axis=0, keepdims=True))

    def by_head(rows):
        return jnp.concatenate([rows[:, h * DK:(h + 1) * DK] for h in range(heads)], axis=0)

    yt[y] = by_head(jnp.concatenate(totals, axis=0))
    pl.when(corner & jnp.logical_not(early))(greet_column)
    under = (y == 0) & (z > 0)

    @pl.when(under)
    def _():
        pl.semaphore_wait(barrier, NY - 1 + nz - 2)

    @pl.when(y > 0)
    def _():
        pl.semaphore_wait(barrier, NY - 1 + nz - 1)

    yt_copies = [
        remote(yt.at[y], yt.at[y], sent, yt_recv, at(z, p)) for i, p in enumerate(y_peers)
    ]
    for copy in yt_copies:
        copy.start()
    for j in range(1, nz - 1):
        pl.when(z > j)(remote(yt.at[y], ct.at[z], sent, ct_recv.at[z], at(j, y)).start)

    rows_at = lax.broadcasted_iota(jnp.int32, (span, 2 * span), 0)
    cols_at = lax.rem(lax.broadcasted_iota(jnp.int32, (span, 2 * span), 1), span)
    own = DK // (NY * nz)
    upper = jnp.where(cols_at > rows_at, 1.0, 0.0).astype(BF16)

    pair = y + 1 - 2 * lax.rem(y, 2)
    across = NY - 1 - y
    first, second = [], []
    for s in range(seqs):
        first.append(pair if s % 2 == 0 else across)
        second.append(across if s % 2 == 0 else pair)

    far_copies, near_copies = [], []
    for s in range(seqs):
        rows = pl.ds(s * span, span)
        left = dot(upper, decays[s])
        vals = acc[rows, width:2 * width].astype(BF16)
        weighted = (inflow[rows, :] * jnp.exp(left)).astype(BF16)
        for h in range(heads):
            lanes = slice(h * DK, (h + 1) * DK)
            state = dot(weighted[:, lanes], vals[:, lanes], ((0,), (0,)))
            high, low = halves(state)
            split[s, 0:DK, lanes] = high
            split[s, DK:2 * DK, lanes] = low
            for zz in range(nz):
                for yy in range(NY):
                    k = (zz * NY + yy) * own
                    ys[yy, s, zz, h * own:(h + 1) * own, :] = state[k:k + own, :]
    for s in range(seqs):
        p = first[s]
        beyond = NY - 1 - p if s % 2 == 0 else p + 1 - 2 * lax.rem(p, 2)
        copy = remote(ys.at[beyond, s], r1.at[s, 1], sent, r1_recv.at[s], at(z, p))
        copy.start()
        far_copies.append(copy)
    for s in range(seqs):
        p = first[s]
        copy = remote(ys.at[p, s], r1.at[s, 0], sent, r2_recv.at[s], at(z, p))
        copy.start()
        near_copies.append(copy)

    for c in range(CHUNKS):
        part = dot(nexts[:, cut(c)], w[cut(c), :])
        next_pre = part if c == 0 else next_pre + part
    forget_pre, next_vals = next_pre[:, 0:width], next_pre[:, width:2 * width]
    next_flow = leak_row * jax.nn.sigmoid(-forget_pre)
    queries = query[...].astype(F32)
    through = by_head(queries * (1.0 - next_flow))
    direct = jnp.sum(by_head(queries * next_flow), axis=1, keepdims=True) * by_head(
        next_vals.astype(BF16).astype(F32)
    )

    arrive(yt.at[0:NY - 1], yt_recv)
    all_y = [yt[j] for j in range(NY)]
    zt[z] = sum(all_y[1:], all_y[0])
    zt_copies = [
        remote(zt.at[z], zt.at[z], sent, zt_recv.at[z], at(p, y)) for i, p in enumerate(z_peers)
    ]
    pl.when(jnp.logical_not(under))(zt_copies[0].start)
    for copy in zt_copies[1:]:
        copy.start()

    @pl.when(under)
    def _():
        pl.semaphore_wait(corner_in, 1)
        zt_copies[0].start()


    def after(p):
        return jnp.exp(sum(jnp.where(p < j, all_y[j], 0.0) for j in range(1, NY)))

    units = seqs * heads
    here = after(y)
    near_src[0:units, :] = here
    near_src[units:2 * units, :] = after(pair)
    near_src[2 * units:3 * units, :] = after(across)
    near_src[3 * units:4 * units, :] = jnp.zeros_like(here)
    near[...] = jnp.transpose(near_src[...])

    def spread(rows, lanes):
        return jnp.concatenate([jnp.broadcast_to(rows[:, c:c + 1], (own, DV)) for c in lanes], axis=0)

    def near_scale(target, which, s):
        return [
            spread(near[pl.ds((j * NY + target) * own, own), :], [which * units + h * seqs + s for h in range(heads)])
            for j in range(nz)
        ]

    def read_segments(later_z):
        weights = through * here * jnp.exp(later_z)
        high, low = halves(weights)
        packed[...] = jnp.concatenate([jnp.concatenate([high, low], axis=0)] * 2, axis=1)
        parts = [None] * units
        for s in range(seqs):
            got = dot(packed[...], split[s])
            for h in range(heads):
                u = h * seqs + s
                lanes = slice(h * DK, (h + 1) * DK)
                parts[u] = got[u:u + 1, lanes] + got[units + u:units + u + 1, lanes]
        rz[z] = jnp.concatenate(parts, axis=0)
        for p in z_peers:
            remote(rz.at[z], rz.at[z], sent, rz_recv, at(p, y)).start()

    def add_arrived(totals, sems):
        def add(j, total):
            arrive(totals.at[j], sems.at[j])
            return total + totals[j]

        return lax.fori_loop(z + 1, nz, add, jnp.zeros_like(through))

    def share_later():
        lt[y] = add_arrived(ct, ct_recv)
        for p in y_peers:
            remote(lt.at[y], lt.at[y], sent, lt_recv, at(z, p)).start()

    top, upper_half, inner = z == nz - 1, z >= nz // 2, (z > 0) & (z < nz - 1)

    @pl.when(top)
    def _():
        read_segments(jnp.zeros_like(through))

    pl.when(inner & upper_half)(share_later)

    r2_copies = []
    for s in range(seqs):
        mine, theirs = near_scale(second[s], 0, s), near_scale(second[s], 1 + s % 2, s)
        far_copies[s].wait_recv()
        for j in range(nz):
            q2[s, j] = mine[j] * ys[second[s], s, j] + theirs[j] * r1[s, 1, j]
        copy = remote(q2.at[s], r2.at[s], sent, r2_recv.at[s], at(z, second[s]))
        copy.start()
        r2_copies.append(copy)

    pl.when(inner & jnp.logical_not(upper_half))(share_later)

    def send_state(p):
        remote(zs.at[p], zr.at[z], sent, zr_recv, at(p, y)).start()

    def prepare_states():
        for s in range(seqs):
            mine, theirs = near_scale(y, 0, s), near_scale(y, 1 + s % 2, s)
            arrive(r1.at[s], r2_recv.at[s])
            for j in range(nz):
                zs[j, s] = (mine[j] * ys[y, s, j] + theirs[j] * r1[s, 0, j]) + r2[s, j]
            zr[z, s] = zs[z, s]
        for p in z_peers[:2]:
            send_state(p)

    soon = (z > 0) & (z < nz // 2)
    pl.when(soon)(prepare_states)

    @pl.when(inner)
    def _():
        arrive(lt.at[0:NY - 1], lt_recv)
        read_segments((lt[0] + lt[1]) + (lt[2] + lt[3]))

    @pl.when(z == 0)
    def _():
        read_segments(add_arrived(zt, zt_recv))

    pl.when(jnp.logical_not(soon))(prepare_states)
    for p in z_peers[2:]:
        send_state(p)

    def await_rest(j, carry):
        arrive(zt.at[j], zt_recv.at[j])
        return carry

    lax.fori_loop(0, z, await_rest, 0)

    @pl.when(z > 0)
    def _():
        lax.fori_loop(z + 1, nz, await_rest, 0)

    running = jnp.zeros_like(through)
    for j in reversed(range(nz)):
        cols_src[j * units:(j + 1) * units, :] = jnp.exp(running)
        running = running + zt[j]
    cols[...] = jnp.transpose(cols_src[...])
    mine = cols[pl.ds(me * own, own), :]

    def column(j, s):
        return spread(mine, [j * units + h * seqs + s for h in range(heads)])

    scale = [[column(j, s) for s in range(seqs)] for j in range(nz)]
    arrive(rz.at[0:nz - 1], rz_recv)
    column_read = rz[0]
    for j in range(1, nz):
        column_read = column_read + rz[j]
    yr[y] = column_read
    for p in y_peers:
        remote(yr.at[y], yr.at[y], sent, yr_recv, at(z, p)).start()

    arrive(zr.at[0:nz - 1], zr_recv)
    for s in range(seqs):
        total = scale[0][s] * zr[0, s]
        for j in range(1, nz):
            total = total + scale[j][s] * zr[j, s]
        cache_out[s] = total.astype(BF16)

    arrive(yr.at[0:NY - 1], yr_recv)
    raw = direct + ((yr[0] + yr[1]) + (yr[2] + yr[3]))
    gain_row = gain[...]
    gains = jnp.concatenate(
        [jnp.broadcast_to(gain_row[:, h * DV:(h + 1) * DV], (seqs, DV)) for h in range(heads)], axis=0
    )
    normed = raw * lax.rsqrt(jnp.mean(raw * raw, axis=1, keepdims=True) + EPS) * gains
    read_out[...] = jnp.concatenate(
        [normed[h * seqs:(h + 1) * seqs, :] for h in range(heads)], axis=1
    ).astype(BF16)

    arrive(yt.at[0:NY - 1], sent)

    def await_sent(j, carry):
        arrive(ct.at[0], sent)
        return carry

    lax.fori_loop(1, z, await_sent, 0)

    @pl.when(inner)
    def _():
        arrive(lt.at[0:NY - 1], sent)

    arrive(zt.at[0:nz - 1], sent)
    for i in range(2):
        arrive(r1.at[:, i], sent)
    arrive(r2, sent)
    arrive(zr.at[0:nz - 1], sent)
    arrive(yr.at[0:NY - 1], sent)
    arrive(rz.at[0:nz - 1], sent)


def local(prompt, forget_weight, value_weight, leak, query, next_input, read_gain):
    seqs, span, depth = prompt.shape
    width = forget_weight.shape[1]
    heads = width // DK
    nz = lax.axis_size("sp") // NY
    own = DK // (NY * nz)
    units = seqs * heads
    dma = pltpu.SemaphoreType.DMA
    anywhere = pl.BlockSpec(memory_space=pl.ANY)
    cache, read = pl.pallas_call(
        functools.partial(kernel, nz),
        out_shape=(
            pltpu.VMEM((seqs, heads * own, DV), BF16),
            pltpu.VMEM((seqs, width), BF16),
        ),
        in_specs=[anywhere] * 7,
        out_specs=(pl.BlockSpec(memory_space=pltpu.VMEM), pl.BlockSpec(memory_space=pltpu.VMEM)),
        scratch_shapes=[
            pltpu.VMEM((seqs * span, depth), BF16),
            pltpu.VMEM((depth, 2 * width), BF16),
            pltpu.VMEM((1, width), F32),
            pltpu.VMEM((seqs, width), BF16),
            pltpu.VMEM((seqs, depth), BF16),
            pltpu.VMEM((1, width), F32),
            pltpu.VMEM((seqs * span, 2 * width), F32),
            pltpu.VMEM((seqs * span, width), F32),
            pltpu.VMEM((seqs, 2 * span, width), BF16),
            pltpu.VMEM((2 * units, 2 * DK), BF16),
            pltpu.VMEM((NY, seqs, nz, heads * own, DV), F32),
            pltpu.VMEM((seqs, 2 * DK, width), BF16),
            pltpu.VMEM((seqs, 2, nz, heads * own, DV), F32),
            pltpu.VMEM((seqs, nz, heads * own, DV), F32),
            pltpu.VMEM((seqs, nz, heads * own, DV), F32),
            pltpu.VMEM((nz, seqs, heads * own, DV), F32),
            pltpu.VMEM((nz, seqs, heads * own, DV), F32),
            pltpu.VMEM((NY, units, DK), F32),
            pltpu.VMEM((nz, units, DK), F32),
            pltpu.VMEM((NY, units, DK), F32),
            pltpu.VMEM((nz, units, DK), F32),
            pltpu.VMEM((NY, units, DV), F32),
            pltpu.VMEM((nz, units, DV), F32),
            pltpu.VMEM((DK, nz * units), F32),
            pltpu.VMEM((nz * units, DK), F32),
            pltpu.VMEM((DK, 4 * units), F32),
            pltpu.VMEM((4 * units, DK), F32),
            dma((CHUNKS,)),
            dma((4,)),
            pltpu.SemaphoreType.REGULAR,
            dma,
            dma,
            dma((nz,)),
            dma,
            dma((nz,)),
            dma((seqs,)),
            dma((seqs,)),
            dma,
            dma,
            dma,
        ],
        compiler_params=pltpu.CompilerParams(
            collective_id=0, has_side_effects=True, vmem_limit_bytes=60 * 1024 * 1024
        ),
    )(
        prompt.reshape(seqs * span, depth),
        forget_weight,
        value_weight,
        leak.reshape(1, width),
        query,
        next_input,
        read_gain.reshape(1, width),
    )
    return cache.reshape(seqs, heads, own, DV), read


def solution(mesh):
    placed = (
        P("gr", "sp", None),
        P(None, "tp"),
        P(None, "tp"),
        P("tp"),
        P("gr", "tp"),
        P("gr", None),
        P("tp"),
    )
    return jax.shard_map(
        local,
        mesh=mesh,
        in_specs=placed,
        out_specs=(P("gr", "tp", "sp", None), P("gr", "tp")),
        check_vma=False,
    )
```
